256 devices in a mesh: ep: 64 (over z, x, core), tp: 4 (over y).
Axes of the slice: x: 4, y: 4, z: 8, core: 2. Of those that a mesh axis runs over, the one named last changes fastest.
Arguments:
- queries: bfloat16 [32768, 8, 96], P('ep', 'tp'), may hold values from -240 to 240
- kv_latent: bfloat16 [32768, 128], P(('ep', 'tp')), may hold values from -6 to 6
- rope_key: bfloat16 [32768, 32], P(('ep', 'tp')), may hold values from -6 to 6
- kv_gain: float32 [128], replicated, may hold values from 0.1 to 1.9
- kv_up: bfloat16 [128, 8, 128], P(None, 'tp'), may hold values from -0.5 to 0.5
- mix_out: bfloat16 [8, 64, 2048], P('tp'), may hold values from -0.25 to 0.25
- moe_in: bfloat16 [16384, 2048], P('ep', 'tp'), may hold values from -6 to 6
- moe_gain: float32 [2048], replicated, may hold values from 0.1 to 1.9
- routes: int32 [16384, 2], P('ep'), may hold values from 0 to 63, all different within a row; in each aligned block of 256 rows (0 to 255, 256 to 511, ...) at most 9 rows name the same one
- route_weights: float32 [16384, 2], P('ep'), may hold values from 0.1 to 1
- gate_w: bfloat16 [64, 2048, 3584], P('ep', None, 'tp'), may hold values from -0.125 to 0.125
- up_w: bfloat16 [64, 2048, 3584], P('ep', None, 'tp'), may hold values from -0.125 to 0.125
- down_w: bfloat16 [64, 3584, 2048], P('ep', 'tp'), may hold values from -0.09375 to 0.09375
Outputs:
- mixed: bfloat16 [32768, 2048], P(('ep', 'tp'))
- moe_out: bfloat16 [16384, 2048], P('ep', 'tp')
The draws below stay inside these ranges and needn't reach their ends.
Inputs may be any that keep to these rules, and one draw needn't show every extreme that they name: `routes`: among the rows of one index of ep, no expert is named by more than 9 entries, a bound that some block reaches; a row names 2 different experts.
All inputs are finite; a program needn't handle non-finite values.
Results may differ from the reference program's by a relative error of at most 0.025.
Values may be sent and summed in bfloat16 or wider, within the bound.
No kernel may reach another device: no remote copies, remote signals or barrier semaphores. Data moves between devices by JAX's collectives and lax.ppermute only.
A program may use at most 128 MiB of HBM per device.

```python
import math
import jax
import jax.numpy as jnp
import numpy as np
from jax import lax

D = 2048
HEADS = 8
NOPE = 64
ROPE = 32
VDIM = 64
KVLAT = 128
FFE = 3584
TOP = 2
EXPERTS = 64
TOKENS_A = 32768
SEQ_LEN = 32768
ROWS_E = 256
TOKENS_E = 16384
CAP = 9
N_EP = 64
N_TP = 4


def draw_queries(key, part):
    base_key = jax.random.fold_in(jax.random.fold_in(key, 11), 0)
    draw_shape = (TOKENS_A, HEADS, NOPE + ROPE)
    normal_part = jnp.clip(jax.random.normal(base_key, draw_shape, jnp.float32), -4.0, 4.0)
    return normal_part.astype(jnp.bfloat16)


def levels(stream_key, shape, cuts, low, high):
    def one(dim, shards_of):
        steps = jax.random.uniform(jax.random.fold_in(jax.random.fold_in(stream_key, 6), dim), (shards_of,), jnp.float32, low / len(cuts), high / len(cuts))
        return jnp.repeat(jnp.exp(steps), shape[dim] // shards_of).reshape((-1,) + (1,) * (len(shape) - dim - 1))

    level = one(*cuts[0])
    for cut in cuts[1:]:
        level = level * one(*cut)
    return level


def assign_block(key, own, number, rows, amount, top, reach, slope):
    ranking = jax.random.permutation(key, amount)
    crowded, ordinary = load_shares(amount, rows * top, reach, slope, True), load_shares(amount, rows * top, reach, slope, False)
    places = jnp.arange(amount)

    def named(tallies, offset_by):
        used = int((tallies > 0).sum())
        fixed = max(1, used // 4)
        moved = fixed + (places - fixed + offset_by * (used - fixed)) % max(1, amount - fixed)
        return jnp.zeros((amount,), jnp.int32).at[ranking[jnp.where(places < fixed, places, moved)]].set(jnp.asarray(tallies, jnp.int32))

    tallies = jnp.where(number % 4 == 0, named(crowded, number // 4), named(ordinary, number - number // 4 - 1))
    mixed = jax.random.permutation(jax.random.fold_in(own, 3), amount)
    source_of, receiver = mixed[0:amount // 2 * 2:2], mixed[1:amount // 2 * 2:2]
    room = jnp.minimum(tallies[source_of] - 1, reach - tallies[receiver]) // 2
    room = jnp.where((source_of == ranking[0]) | (receiver == ranking[0]) | (tallies[receiver] == 0), 0, jnp.maximum(room, 0))
    moved = jax.random.randint(jax.random.fold_in(own, 4), (amount // 2,), 0, 1 << 20) % (room + 1)
    tallies = tallies.at[source_of].add(-moved).at[receiver].add(moved)
    items = jnp.searchsorted(jnp.cumsum(tallies), jnp.arange(rows * top), side="right").astype(jnp.int32)
    listing = items.reshape(top, rows).T
    listing = listing[jax.random.permutation(jax.random.fold_in(own, 1), rows)]
    offset_by = jax.random.randint(jax.random.fold_in(own, 2), (rows, 1), 0, top)
    return jnp.take_along_axis(listing, (jnp.arange(top)[None, :] + offset_by) % top, axis=1)


def load_shares(count, total, limit, lean, full):
    weights = [(1 << 20) // math.isqrt(grade ** lean) + 1 for grade in range(1, count + 1)]
    largest = limit if full else min(limit, max(-(-total // count), total * weights[0] // sum(weights)))
    least = 1 if total - largest >= count - 1 else 0
    given, rest = [largest] + [least] * (count - 1), total - largest - least * (count - 1)
    while rest > 0:
        candidates = [i for i in range(1, count) if given[i] < largest] or [i for i in range(1, count) if given[i] < limit]
        mass, remaining = sum([weights[i] for i in candidates]), rest
        for i in candidates:
            extra = min(limit - given[i], max(1, remaining * weights[i] // mass), rest)
            given[i] = given[i] + extra
            rest = rest - extra
    return np.array(given)


def scatter_about(own_key, dims, deviation, most, pieces=(), kind=jnp.bfloat16):
    array = deviation * jax.random.normal(own_key, dims, jnp.float32)
    if pieces:
        array = array * levels(own_key, dims, pieces, -0.22, 0.18)
    return jnp.clip(array, -most, most).astype(kind)


def setup_inputs(seed: int = 0) -> dict:
    seeds = jax.random.split(jax.random.key(seed), 14)
    queries = draw_queries(jax.random.fold_in(seeds[13], 71), 0)
    kv_latent = scatter_about(seeds[1], (TOKENS_A, KVLAT), 1.0, 6.0, ((0, 256),))
    rope_key = scatter_about(seeds[2], (TOKENS_A, ROPE), 1.0, 6.0, ((0, 256),))
    kv_gain = jnp.clip(1.0 + 0.18 * jax.random.normal(seeds[3], (KVLAT,), jnp.float32), 0.1, 1.9)
    kv_up = scatter_about(seeds[4], (KVLAT, HEADS, NOPE + VDIM), KVLAT ** -0.5, 0.5, ((1, 4),))
    mix_out = scatter_about(seeds[5], (HEADS, VDIM, D), (HEADS * VDIM) ** -0.5, 0.25, ((0, 4),))
    moe_in = scatter_about(seeds[6], (TOKENS_E, D), 1.0, 6.0, ((0, 64), (1, 4)))
    moe_gain = jnp.clip(1.0 + 0.18 * jax.random.normal(seeds[7], (D,), jnp.float32), 0.1, 1.9)
    routes_keys = jax.random.split(jax.random.fold_in(seeds[8], 1), TOKENS_E // ROWS_E)
    routes_turns = jax.random.permutation(jax.random.fold_in(seeds[8], 3), TOKENS_E // ROWS_E)
    routes = jax.vmap(lambda own, number: assign_block(jax.random.fold_in(seeds[8], 2), own, number, ROWS_E, EXPERTS, TOP, CAP, 1))(routes_keys, routes_turns).reshape((TOKENS_E, TOP))
    route_weights = jnp.clip(0.1 + 0.9 * jax.random.uniform(seeds[9], (TOKENS_E, TOP), jnp.float32) ** levels(seeds[9], (TOKENS_E, TOP), ((0, 64),), -0.2, 0.2), 0.1, 1.0)
    gate_w = scatter_about(seeds[10], (EXPERTS, D, FFE), D ** -0.5, 0.125, ((0, 64), (2, 4)))
    up_w = scatter_about(seeds[11], (EXPERTS, D, FFE), D ** -0.5, 0.125, ((0, 64), (2, 4)))
    down_w = scatter_about(seeds[12], (EXPERTS, FFE, D), FFE ** -0.5, 0.09375, ((0, 64), (1, 4)))
    return dict(queries=queries, kv_latent=kv_latent, rope_key=rope_key, kv_gain=kv_gain, kv_up=kv_up, mix_out=mix_out, moe_in=moe_in, moe_gain=moe_gain, routes=routes, route_weights=route_weights, gate_w=gate_w, up_w=up_w, down_w=down_w)


eps = 1e-06
rope_base = 10000.0
neg_big = -1e+30

def rotate(values, positions):
    half_dim = values.shape[-1] // 2
    inv_freq = rope_base ** (-jnp.arange(half_dim, dtype=jnp.float32) * 2.0 / values.shape[-1])
    angles = positions.astype(jnp.float32)[:, None] * inv_freq[None, :]
    angles = angles.reshape((angles.shape[0],) + (1,) * (values.ndim - 2) + (half_dim,))
    cosine = jnp.cos(angles)
    sine_part = jnp.sin(angles)
    first_half = values[..., :half_dim].astype(jnp.float32)
    second_half = values[..., half_dim:].astype(jnp.float32)
    return jnp.concatenate([first_half * cosine - second_half * sine_part, second_half * cosine + first_half * sine_part], axis=-1)

def slot_table(block_routes):
    flat_routes = block_routes.reshape(-1)
    onehot = (flat_routes[:, None] == jnp.arange(EXPERTS, dtype=jnp.int32)[None, :]).astype(jnp.int32)
    slot_rank = lax.optimization_barrier(jnp.sum((jnp.cumsum(onehot, axis=0) - onehot) * onehot, axis=1))
    slot_dest = flat_routes * CAP + slot_rank
    slot_owner = jnp.full((EXPERTS * CAP,), -1, jnp.int32).at[slot_dest].set(jnp.arange(flat_routes.shape[0], dtype=jnp.int32))
    return (slot_dest, slot_owner)

def reference(queries, kv_latent, rope_key, kv_gain, kv_up, mix_out, moe_in, moe_gain, routes, route_weights, gate_w, up_w, down_w):
    total_rows = queries.shape[0]
    token_index = jnp.arange(total_rows, dtype=jnp.int32)
    positions = token_index % SEQ_LEN
    query_nope = queries[..., :NOPE]
    query_rot = rotate(queries[..., NOPE:], positions).astype(jnp.bfloat16)
    latent_f = kv_latent.astype(jnp.float32)
    normed = (latent_f * lax.rsqrt(lax.optimization_barrier(jnp.mean(latent_f * latent_f, axis=-1, keepdims=True)) + eps) * kv_gain).astype(jnp.bfloat16)
    head_proj = jnp.einsum('nr,rhd->nhd', normed.astype(jnp.float32), kv_up.astype(jnp.float32)).astype(jnp.bfloat16)
    key_nope = head_proj[..., :NOPE]
    values = head_proj[..., NOPE:]
    key_rot = rotate(rope_key, positions).astype(jnp.bfloat16)
    query_block = min(512, SEQ_LEN)
    score_scale = 1.0 / math.sqrt(NOPE + ROPE)

    def attend_block(first_row):
        seq_start = first_row // SEQ_LEN * SEQ_LEN
        block_nope = lax.dynamic_slice_in_dim(query_nope, first_row, query_block, 0).astype(jnp.float32)
        block_rot = lax.dynamic_slice_in_dim(query_rot, first_row, query_block, 0).astype(jnp.float32)
        seq_nope = lax.dynamic_slice_in_dim(key_nope, seq_start, SEQ_LEN, 0).astype(jnp.float32)
        seq_rot = lax.dynamic_slice_in_dim(key_rot, seq_start, SEQ_LEN, 0).astype(jnp.float32)
        seq_values = lax.dynamic_slice_in_dim(values, seq_start, SEQ_LEN, 0).astype(jnp.float32)
        scores = (jnp.einsum('qhd,khd->qhk', block_nope, seq_nope) + jnp.einsum('qhd,kd->qhk', block_rot, seq_rot)) * score_scale
        query_ids = first_row + jnp.arange(query_block, dtype=jnp.int32)
        key_ids = seq_start + jnp.arange(SEQ_LEN, dtype=jnp.int32)
        allowed = (key_ids[None, :] <= query_ids[:, None])[:, None, :]
        scores = jnp.where(allowed, scores, neg_big)
        row_max = lax.optimization_barrier(jnp.max(scores, axis=-1, keepdims=True))
        probs = jnp.where(allowed, jnp.exp(scores - row_max), 0.0)
        denom = lax.optimization_barrier(jnp.sum(probs, axis=-1))
        weighted = jnp.einsum('qhk,khd->qhd', probs.astype(jnp.bfloat16).astype(jnp.float32), seq_values)
        return (weighted / denom[..., None]).astype(jnp.bfloat16)
    starts = jnp.arange(0, total_rows, query_block, dtype=jnp.int32)
    attn = lax.map(attend_block, starts).reshape(total_rows, HEADS, VDIM)
    group_heads = HEADS // N_TP
    mixed = jnp.zeros((total_rows, D), jnp.float32)
    for group in range(N_TP):
        part_sum = jnp.einsum('thv,hvd->td', attn[:, group * group_heads:(group + 1) * group_heads].astype(jnp.float32), mix_out[group * group_heads:(group + 1) * group_heads].astype(jnp.float32))
        rounded = lax.optimization_barrier(part_sum.astype(jnp.bfloat16))
        mixed = mixed + rounded.astype(jnp.float32)
    mixed = mixed.astype(jnp.bfloat16)
    slot_dest, slot_owner = jax.vmap(slot_table)(routes.reshape(N_EP, ROWS_E, TOP))
    moe_f = moe_in.astype(jnp.float32)
    row_scale = lax.rsqrt(lax.optimization_barrier(jnp.mean(moe_f * moe_f, axis=-1)) + eps)
    scaled = (moe_f * moe_gain).astype(jnp.bfloat16)
    owner_by_expert = slot_owner.reshape(N_EP, EXPERTS, CAP).transpose(1, 0, 2)
    block_base = (jnp.arange(N_EP, dtype=jnp.int32) * ROWS_E)[:, None]
    quarter = FFE // N_TP

    def serve_expert(inputs):
        expert, slots = inputs
        is_valid = (slots >= 0).reshape(-1)
        token_row = (block_base + jnp.maximum(slots, 0) // TOP).reshape(-1)
        picked_rows = scaled[token_row].astype(jnp.float32)
        picked_scale = row_scale[token_row][:, None]
        gate = jnp.dot(picked_rows, gate_w[expert].astype(jnp.float32)) * picked_scale
        up_val = jnp.dot(picked_rows, up_w[expert].astype(jnp.float32)) * picked_scale
        hidden = (jax.nn.silu(gate) * up_val).astype(jnp.bfloat16)
        down_expert = down_w[expert]
        expert_sum = jnp.zeros((hidden.shape[0], D), jnp.float32)
        for group in range(N_TP):
            part_sum = jnp.dot(hidden[:, group * quarter:(group + 1) * quarter].astype(jnp.float32), down_expert[group * quarter:(group + 1) * quarter].astype(jnp.float32))
            rounded = lax.optimization_barrier(part_sum.astype(jnp.bfloat16))
            expert_sum = expert_sum + rounded.astype(jnp.float32)
        return jnp.where(is_valid[:, None], expert_sum, 0.0).astype(jnp.bfloat16)
    results = lax.map(serve_expert, (jnp.arange(EXPERTS, dtype=jnp.int32), owner_by_expert)).reshape(EXPERTS, N_EP, CAP, D)
    route_flat = routes.reshape(N_EP, ROWS_E * TOP)
    slot_pos = slot_dest - route_flat * CAP
    block_ids = jnp.broadcast_to(jnp.arange(N_EP, dtype=jnp.int32)[:, None], route_flat.shape)
    picked = results[route_flat, block_ids, slot_pos].astype(jnp.float32).reshape(TOKENS_E, TOP, D)
    moe_out = lax.optimization_barrier(jnp.sum(picked * route_weights[..., None], axis=1)).astype(jnp.bfloat16)
    return (mixed, moe_out)
```

```python
import math

import jax
import jax.numpy as jnp
from jax import lax
from jax.experimental import pallas as pl
from jax.experimental.pallas import tpu as pltpu
from jax.sharding import Mesh
from jax.sharding import PartitionSpec as P

BF = jnp.bfloat16
F32 = jnp.float32
D = 2048
NOPE = 64
ROPE = 32
VDIM = 64
KVLAT = 128
N_EP = 64
N_TP = 4
HALF = 256
PIECE = 128
TILE = 4
ROWS = 256
SLOTS = 10
EP = ("z", "x", "c")
ALL = ("z", "x", "c", "tp")

eps = 1e-06
rope_base = 10000.0
neg_big = -1e30
score_scale = math.log2(math.e) / math.sqrt(NOPE + ROPE)


def ring(count, step):
    return [(i, (i + step) % count) for i in range(count)]


def rotate(values, positions):
    half_dim = values.shape[-1] // 2
    inv_freq = rope_base ** (-jnp.arange(half_dim, dtype=F32) * 2.0 / values.shape[-1])
    angles = positions.astype(F32)[:, None] * inv_freq[None, :]
    angles = angles.reshape((angles.shape[0],) + (1,) * (values.ndim - 2) + (half_dim,))
    cosine = jnp.cos(angles)
    sine_part = jnp.sin(angles)
    first_half = values[..., :half_dim].astype(F32)
    second_half = values[..., half_dim:].astype(F32)
    return jnp.concatenate(
        [
            first_half * cosine - second_half * sine_part,
            second_half * cosine + first_half * sine_part,
        ],
        axis=-1,
    )


def attend_body(where, k0, k1, k2, k3, k4, k5, k6, k7, first, second, out, kbuf, vbuf, wk, wv, qs, tops, acc, sbuf, allkeys):
    ep = where[0]
    tp = where[1]
    z = where[2]
    x = where[3]
    c = where[4]
    short = jnp.minimum(ep, N_EP - 1 - ep)
    n_short = short // TILE
    n_long = (N_EP - 1 - short) // TILE
    long_half = jnp.where(ep < N_EP // 2, 1, 0)
    heads = 4
    pieces = (first, second)
    for n, part in enumerate((k0, k1, k2, k3, k4, k5, k6, k7)):
        allkeys[8 * n : 8 * n + 8] = part[...]
    row = lax.broadcasted_iota(jnp.int32, (ROPE, 128), 0)
    lane = lax.broadcasted_iota(jnp.int32, (ROPE, 128), 1)
    pass_rope = jnp.where(lane == row + NOPE, 1.0, 0.0).astype(BF)
    lane = lax.broadcasted_iota(jnp.int32, (KVLAT, 128), 1)
    for h in range(heads):
        up = pieces[h // 2][384:512, (h % 2) * 128 : (h % 2 + 1) * 128]
        wk[:KVLAT, h * 128 : (h + 1) * 128] = jnp.where(lane < NOPE, up, jnp.zeros_like(up))
        wk[KVLAT:, h * 128 : (h + 1) * 128] = pass_rope
        wv[h * VDIM : (h + 1) * VDIM, :] = up.T[NOPE:, :]
    for half in range(2):
        for h in range(heads):
            at = (half * 2 + h % 2) * 96
            q = pieces[h // 2][at : at + 96, :].astype(F32) * score_scale
            high = q.astype(BF)
            low = (q - high.astype(F32)).astype(BF)
            pad = jnp.zeros((32, HALF), BF)
            qs[half, h] = jnp.concatenate([high, pad, low, pad], axis=0)
    tops[...] = jnp.full(tops.shape, neg_big, F32)
    acc[...] = jnp.zeros(acc.shape, F32)

    def project(t, _):
        blocks = []
        for b in range(TILE):
            zb = t // 2
            xb = (t % 2) * 2 + b // 2
            cb = b % 2
            at = ((c + cb) % 2) * 32 + ((x - xb) % 4) * 8 + (z - zb) % 8
            blocks.append(allkeys[at])
        turned = jnp.concatenate(blocks, axis=1)
        kbuf[t] = jnp.dot(turned.T, wk[...], preferred_element_type=F32).astype(BF)
        vbuf[t] = jnp.dot(wv[...], turned[:KVLAT], preferred_element_type=F32).astype(BF)
        return 0

    lax.fori_loop(0, n_long + 1, project, 0)
    ones = jnp.ones((16, TILE * PIECE), BF)

    def tile(t, half, at_edge):
        if at_edge:
            r = lax.broadcasted_iota(jnp.int32, (TILE * PIECE, HALF), 0)
            q = lax.broadcasted_iota(jnp.int32, (TILE * PIECE, HALF), 1)
            block = jnp.where(half == 0, ep, N_EP - 1 - ep)
            first_key = (r // PIECE) * 512 + r % PIECE
            allowed = (first_key - q) <= 512 * block + HALF * half - 2048 * t - PIECE * tp
        for h in range(heads):
            k = kbuf[t, :, h * 128 : (h + 1) * 128]
            scores = jnp.dot(
                jnp.concatenate([k, k], axis=1), qs[half, h], preferred_element_type=F32
            )
            if at_edge:
                scores = jnp.where(allowed, scores, neg_big)
            sbuf[h] = scores
        for h in range(heads):
            scores = sbuf[h]
            old = tops[half, h, 0:1, :]
            new = jnp.maximum(old, jnp.max(scores, axis=0, keepdims=True))
            probs = jnp.exp2(scores - new)
            if at_edge:
                probs = jnp.where(allowed, probs, 0.0)
            v = jnp.concatenate([vbuf[t, h * VDIM : (h + 1) * VDIM, :], ones], axis=0)
            part = jnp.dot(v, probs.astype(BF), preferred_element_type=F32)
            acc[half, h] = acc[half, h] * jnp.exp2(old - new) + part
            tops[half, h, 0:1, :] = new

    def inner(w, _):
        is_long = w < n_long
        tile(
            jnp.where(is_long, w, w - n_long),
            jnp.where(is_long, long_half, 1 - long_half),
            False,
        )
        return 0

    lax.fori_loop(0, n_long + n_short, inner, 0)

    def edge(w, _):
        tile(
            jnp.where(w == 0, n_long, n_short),
            jnp.where(w == 0, long_half, 1 - long_half),
            True,
        )
        return 0

    lax.fori_loop(0, 2, edge, 0)
    for half in range(2):
        parts = ([], [], [])
        for h in range(heads):
            a = acc[half, h]
            total = a[VDIM : VDIM + 1]
            seen = total > 0.0
            safe = jnp.where(seen, total, 1.0)
            o = (a[:VDIM] / safe).astype(BF)
            lse = jnp.where(seen, tops[half, h, 0:1, :] + jnp.log2(safe), neg_big)
            one = lse.astype(BF).astype(F32)
            two = (lse - one).astype(BF).astype(F32)
            parts[0].append(one)
            parts[1].append(two)
            parts[2].append(lse - one - two)
            for cc in range(2):
                to = (2 * half + cc - tp) % N_TP
                out[to, h * VDIM : (h + 1) * VDIM, :] = o[:, cc * 128 : (cc + 1) * 128]
        stats = jnp.concatenate(
            parts[0] + parts[1] + parts[2] + [jnp.zeros((4, HALF), F32)], axis=0
        ).astype(BF)
        for cc in range(2):
            to = (2 * half + cc - tp) % N_TP
            out[to, heads * VDIM :, :] = stats[:, cc * 128 : (cc + 1) * 128]


def attend(where, keys, first, second):
    work = 17 * 4 * TILE * PIECE * HALF
    return pl.pallas_call(
        attend_body,
        out_shape=jax.ShapeDtypeStruct((4, 4 * VDIM + 16, 128), BF),
        in_specs=[pl.BlockSpec(memory_space=pltpu.SMEM)]
        + [pl.BlockSpec(memory_space=pltpu.VMEM)] * 10,
        out_specs=pl.BlockSpec(memory_space=pltpu.VMEM),
        scratch_shapes=[
            pltpu.VMEM((N_EP // TILE, TILE * PIECE, 4 * 128), BF),
            pltpu.VMEM((N_EP // TILE, 4 * VDIM, TILE * PIECE), BF),
            pltpu.VMEM((KVLAT + ROPE, 4 * 128), BF),
            pltpu.VMEM((4 * VDIM, KVLAT), BF),
            pltpu.VMEM((2, 4, 256, HALF), BF),
            pltpu.VMEM((2, 4, 8, HALF), F32),
            pltpu.VMEM((2, 4, VDIM + 16, HALF), F32),
            pltpu.VMEM((4, TILE * PIECE, HALF), F32),
            pltpu.VMEM((N_EP, KVLAT + ROPE, PIECE), BF),
        ],
        compiler_params=pltpu.CompilerParams(vmem_limit_bytes=36 * 1024 * 1024),
        cost_estimate=pl.CostEstimate(
            flops=work * 1000, bytes_accessed=4 << 20, transcendentals=work
        ),
        name="attend",
    )(where, *keys, first, second)


def stack_body(*refs):
    for n, part in enumerate(refs[:-1]):
        refs[-1][n] = part[...]


def stack(parts):
    return pl.pallas_call(
        stack_body,
        out_shape=jax.ShapeDtypeStruct((len(parts), *parts[0].shape), BF),
        in_specs=[pl.BlockSpec(memory_space=pltpu.VMEM)] * len(parts),
        out_specs=pl.BlockSpec(memory_space=pltpu.VMEM),
        cost_estimate=pl.CostEstimate(flops=1 << 20, bytes_accessed=1 << 20, transcendentals=0),
        name="stack",
    )(*parts)


def join_body(*refs):
    out = refs[-1]
    got = refs[:-1]
    for e in range(N_TP):
        for k in range(2):
            lses = []
            vals = []
            for d in range(N_TP):
                g = (e - d) % N_TP
                h = (g % 2) * 2 + k
                ref = got[2 * d + g // 2]
                stats = ref[4 * VDIM : 4 * VDIM + 16, :].astype(F32)
                lses.append(stats[h : h + 1] + stats[4 + h : 5 + h] + stats[8 + h : 9 + h])
                vals.append(ref[h * VDIM : (h + 1) * VDIM, :].astype(F32))
            top = jnp.maximum(jnp.maximum(lses[0], lses[1]), jnp.maximum(lses[2], lses[3]))
            ws = [jnp.exp2(a - top) for a in lses]
            total = ws[0] + ws[1] + ws[2] + ws[3]
            o = ws[0] * vals[0] + ws[1] * vals[1] + ws[2] * vals[2] + ws[3] * vals[3]
            at = e * 128 + k * VDIM
            out[at : at + VDIM, :] = (o / total).astype(BF)


def join(pieces):
    return pl.pallas_call(
        join_body,
        out_shape=jax.ShapeDtypeStruct((512, 128), BF),
        in_specs=[pl.BlockSpec(memory_space=pltpu.VMEM)] * 8,
        out_specs=pl.BlockSpec(memory_space=pltpu.VMEM),
        cost_estimate=pl.CostEstimate(flops=1 << 20, bytes_accessed=1 << 20, transcendentals=0),
        name="join",
    )(*pieces)


def mix_body(attn, w0, w1, w2, w3, out):
    a = attn[...].T
    total = jnp.zeros((128, D), F32)
    for e, w in enumerate((w0, w1, w2, w3)):
        total = total + jnp.dot(
            a[:, e * 128 : (e + 1) * 128], w[...], preferred_element_type=F32
        )
    out[...] = total.astype(BF)


def mix(attn, weights):
    return pl.pallas_call(
        mix_body,
        out_shape=jax.ShapeDtypeStruct((128, D), BF),
        in_specs=[pl.BlockSpec(memory_space=pltpu.VMEM)] * 5,
        out_specs=pl.BlockSpec(memory_space=pltpu.VMEM),
        cost_estimate=pl.CostEstimate(
            flops=2 * 128 * 512 * D, bytes_accessed=3 << 20, transcendentals=0
        ),
        name="mix",
    )(attn, *weights)


def route_body(routes, turned, tokens, send, dest):
    experts = lax.broadcasted_iota(jnp.int32, (ROWS, N_EP), 1)
    a = lax.broadcasted_iota(jnp.int32, (ROWS, ROWS), 0)
    b = lax.broadcasted_iota(jnp.int32, (ROWS, ROWS), 1)
    before = jnp.where(b < a, 1.0, 0.0).astype(BF)
    named = [jnp.where(routes[:, k : k + 1] == experts, 1.0, 0.0) for k in range(2)]
    base = lax.broadcasted_iota(jnp.int32, (1, N_EP), 1).astype(F32) * SLOTS
    for k in range(2):
        rank = jnp.dot(before, named[k].astype(BF), preferred_element_type=F32) + base
        if k:
            rank = rank + jnp.sum(named[0], axis=0, keepdims=True)
        dest[:, k : k + 1] = jnp.sum(rank * named[k], axis=1, keepdims=True).astype(jnp.int32)
    experts = lax.broadcasted_iota(jnp.int32, (N_EP, ROWS), 0)
    before = jnp.where(a < b, 1.0, 0.0).astype(BF)
    named = [jnp.where(turned[k : k + 1, :] == experts, 1.0, 0.0) for k in range(2)]
    base = lax.broadcasted_iota(jnp.int32, (N_EP, 1), 0).astype(F32) * SLOTS
    slot = lax.broadcasted_iota(jnp.int32, (N_EP * SLOTS, ROWS), 0)
    pick = jnp.zeros((N_EP * SLOTS, ROWS), jnp.bool_)
    for k in range(2):
        rank = jnp.dot(named[k].astype(BF), before, preferred_element_type=F32) + base
        if k:
            rank = rank + jnp.sum(named[0], axis=1, keepdims=True)
        to = jnp.sum(rank * named[k], axis=0, keepdims=True).astype(jnp.int32)
        pick = pick | (slot == to)
    pick = jnp.where(pick, 1.0, 0.0).astype(BF)
    send[...] = jnp.dot(pick, tokens[...], preferred_element_type=F32).astype(BF)


def route(routes, tokens):
    return pl.pallas_call(
        route_body,
        out_shape=(
            jax.ShapeDtypeStruct((N_EP * SLOTS, tokens.shape[1]), BF),
            jax.ShapeDtypeStruct((ROWS, 2), jnp.int32),
        ),
        in_specs=[pl.BlockSpec(memory_space=pltpu.VMEM)] * 3,
        out_specs=(pl.BlockSpec(memory_space=pltpu.VMEM),) * 2,
        cost_estimate=pl.CostEstimate(flops=1 << 28, bytes_accessed=1 << 20, transcendentals=0),
        name="route",
    )(routes, routes.T, tokens)


def expert_body(
    where, x0, x1, x2, x3, gain, gate_w, up_w, down_w, out, xs, wg, wu, wd, gate, up, sems
):
    tp = where[1]
    quarter = D // N_TP
    copies = []
    for d in range(N_TP):
        rows = pl.ds(pl.multiple_of(((tp - d) % N_TP) * quarter, quarter), quarter)
        here = slice(d * quarter, (d + 1) * quarter)
        copies.append(
            (
                pltpu.make_async_copy(gate_w.at[0, rows, :], wg.at[d], sems.at[0, d]),
                pltpu.make_async_copy(up_w.at[0, rows, :], wu.at[d], sems.at[1, d]),
            )
        )
    downs = []
    for d in range(N_TP):
        cols = pl.ds(pl.multiple_of(((tp + d) % N_TP) * quarter, quarter), quarter)
        downs.append(pltpu.make_async_copy(down_w.at[0, :, cols], wd.at[d], sems.at[2, d]))
    for pair in copies:
        pair[0].start()
        pair[1].start()
    for copy in downs:
        copy.start()
    squares = jnp.zeros((x0.shape[0], 1), F32)
    for d, x in enumerate((x0, x1, x2, x3)):
        v = x[...].astype(F32)
        squares = squares + jnp.sum(v * v, axis=1, keepdims=True)
        xs[d] = (v * gain[pl.ds((tp - d) % N_TP, 1), :]).astype(BF)
    row_scale = lax.rsqrt(squares / D + eps)
    for d in range(N_TP):
        copies[d][0].wait()
        copies[d][1].wait()
        g = jnp.dot(xs[d], wg[d], preferred_element_type=F32)
        u = jnp.dot(xs[d], wu[d], preferred_element_type=F32)
        if d:
            gate[...] += g
            up[...] += u
        else:
            gate[...] = g
            up[...] = u
    g = gate[...] * row_scale
    hidden = (g / (1.0 + jnp.exp(-g)) * (up[...] * row_scale)).astype(BF)
    for d in range(N_TP):
        downs[d].wait()
        out[d] = jnp.dot(hidden, wd[d], preferred_element_type=F32).astype(BF)


def expert(where, xs, gain, gate_w, up_w, down_w):
    rows = xs[0].shape[0]
    hidden = gate_w.shape[2]
    quarter = D // N_TP
    return pl.pallas_call(
        expert_body,
        out_shape=jax.ShapeDtypeStruct((N_TP, rows, quarter), BF),
        in_specs=[pl.BlockSpec(memory_space=pltpu.SMEM)]
        + [pl.BlockSpec(memory_space=pltpu.VMEM)] * 5
        + [pl.BlockSpec(memory_space=pl.ANY)] * 3,
        out_specs=pl.BlockSpec(memory_space=pltpu.VMEM),
        scratch_shapes=[
            pltpu.VMEM((N_TP, rows, quarter), BF),
            pltpu.VMEM((N_TP, quarter, hidden), BF),
            pltpu.VMEM((N_TP, quarter, hidden), BF),
            pltpu.VMEM((N_TP, hidden, quarter), BF),
            pltpu.VMEM((rows, hidden), F32),
            pltpu.VMEM((rows, hidden), F32),
            pltpu.SemaphoreType.DMA((3, N_TP)),
        ],
        compiler_params=pltpu.CompilerParams(vmem_limit_bytes=40 * 1024 * 1024),
        cost_estimate=pl.CostEstimate(
            flops=6 * rows * D * hidden, bytes_accessed=16 << 20, transcendentals=rows * hidden
        ),
        name="expert",
    )(where, *xs, gain.reshape(N_TP, quarter), gate_w, up_w, down_w)


def weigh_body(dest, weights, back, out):
    slot = lax.broadcasted_iota(jnp.int32, (ROWS, N_EP * SLOTS), 1)
    w = jnp.zeros((ROWS, N_EP * SLOTS), F32)
    for k in range(2):
        w = jnp.where(slot == dest[:, k : k + 1], weights[:, k : k + 1], w)
    high = w.astype(BF)
    rest = w - high.astype(F32)
    mid = rest.astype(BF)
    low = (rest - mid.astype(F32)).astype(BF)
    b = back[...]
    total = jnp.dot(low, b, preferred_element_type=F32)
    total = total + jnp.dot(mid, b, preferred_element_type=F32)
    total = total + jnp.dot(high, b, preferred_element_type=F32)
    out[...] = total.astype(BF)


def weigh(dest, weights, back):
    return pl.pallas_call(
        weigh_body,
        out_shape=jax.ShapeDtypeStruct((ROWS, back.shape[1]), BF),
        in_specs=[pl.BlockSpec(memory_space=pltpu.VMEM)] * 3,
        out_specs=pl.BlockSpec(memory_space=pltpu.VMEM),
        cost_estimate=pl.CostEstimate(flops=1 << 29, bytes_accessed=1 << 20, transcendentals=0),
        name="weigh",
    )(dest, weights, back)


def from_each(value, axis, count):
    return [value] + [lax.ppermute(value, axis, ring(count, d)) for d in range(1, count)]


def shards(
    queries,
    kv_latent,
    rope_key,
    kv_gain,
    kv_up,
    mix_out,
    moe_in,
    moe_gain,
    routes,
    route_weights,
    gate_w,
    up_w,
    down_w,
):
    ep = lax.axis_index(EP)
    tp = lax.axis_index("tp")
    where = jnp.stack(
        [ep, tp, lax.axis_index("z"), lax.axis_index("x"), lax.axis_index("c")]
    ).astype(jnp.int32)

    key_index = ep * 512 + tp * PIECE + jnp.arange(PIECE, dtype=jnp.int32)
    latent = kv_latent.astype(F32)
    normed = (
        latent * lax.rsqrt(jnp.mean(latent * latent, axis=-1, keepdims=True) + eps) * kv_gain
    ).astype(BF)
    key_rot = rotate(rope_key, key_index).astype(BF)
    keys = jnp.concatenate([normed.T, key_rot.T], axis=0)
    keys = stack(from_each(keys, "z", 8))
    keys = from_each(keys, "x", 4)
    keys = keys + [lax.ppermute(k, "c", ring(2, 1)) for k in keys]

    query_index = ep * 512 + jnp.arange(512, dtype=jnp.int32)
    query_rot = rotate(queries[..., NOPE:], query_index).astype(BF)
    q = jnp.concatenate([queries[..., :NOPE], query_rot], axis=-1).transpose(1, 2, 0)
    mirrored = lax.ppermute(q[:, :, HALF:], EP, [(i, N_EP - 1 - i) for i in range(N_EP)])
    bundle = jnp.concatenate(
        [q[:, :, :HALF].reshape(192, HALF), mirrored.reshape(192, HALF), kv_up.reshape(128, 256)],
        axis=0,
    )
    bundles = from_each(bundle, "tp", N_TP)

    send, dest = route(routes, moe_in)
    arrived = lax.all_to_all(
        send.reshape(N_EP, SLOTS * 4, 128), EP, split_axis=0, concat_axis=0, tiled=True
    )
    arrived = arrived.reshape(N_EP * SLOTS, 512)
    arrived, bundles = lax.optimization_barrier((arrived, bundles))
    xs = from_each(arrived, "tp", N_TP)
    part_a = attend(where, keys, bundles[0], bundles[1])
    xs, part_a = lax.optimization_barrier((xs, part_a))
    results = expert(where, xs, moe_gain, gate_w, up_w, down_w)
    results, bundles, mix_in = lax.optimization_barrier((results, bundles, mix_out))
    sums = [results[0]] + [
        lax.ppermute(results[d], "tp", ring(N_TP, d)) for d in range(1, N_TP)
    ]
    part_b = attend(where, keys, bundles[2], bundles[3])
    sums, part_b = lax.optimization_barrier((sums, part_b))
    summed = sum(a.astype(F32) for a in sums).astype(BF)
    back = lax.all_to_all(
        summed.reshape(N_EP, SLOTS * 4, 128), EP, split_axis=0, concat_axis=0, tiled=True
    )
    moe_out = weigh(dest, route_weights, back.reshape(N_EP * SLOTS, 512))

    mix_w = from_each(mix_in.reshape(128, D), "tp", N_TP)
    got = []
    for d in range(N_TP):
        for part in (part_a, part_b):
            got.append(part[0] if d == 0 else lax.ppermute(part[d], "tp", ring(N_TP, d)))
    attn = join(got)
    owners = [
        (i * N_TP + j, (i if j < 2 else N_EP - 1 - i) * N_TP + j)
        for i in range(N_EP)
        for j in range(N_TP)
    ]
    attn = lax.ppermute(attn, ALL, owners)
    mixed = mix(attn, mix_w)
    return (mixed, moe_out)


def solution(mesh):
    split = Mesh(mesh.devices.reshape(8, 4, 2, mesh.shape["tp"]), ALL)
    placed = (
        P(EP, "tp", None),
        P(ALL, None),
        P(ALL, None),
        P(),
        P(None, "tp", None),
        P("tp", None, None),
        P(EP, "tp"),
        P(),
        P(EP, None),
        P(EP, None),
        P(EP, None, "tp"),
        P(EP, None, "tp"),
        P(EP, "tp", None),
    )
    return jax.shard_map(
        shards,
        mesh=split,
        in_specs=placed,
        out_specs=(P(ALL, None), P(EP, "tp")),
        check_vma=False,
    )
```

```python
import math

import jax
import jax.numpy as jnp
from jax import lax
from jax.experimental import pallas as pl
from jax.experimental.pallas import tpu as pltpu
from jax.sharding import Mesh
from jax.sharding import PartitionSpec as P


BF = jnp.bfloat16
F32 = jnp.float32
D = 2048
NOPE = 64
ROPE = 32
VDIM = 64
KVLAT = 128
N_EP = 64
N_TP = 4
HALF = 256
PIECE = 128
TILE = 4
ROWS = 256
SLOTS = 10
EP = ("z", "x", "c")
ALL = ("z", "x", "c", "tp")

eps = 1e-06
rope_base = 10000.0
neg_big = -1e30
score_scale = math.log2(math.e) / math.sqrt(NOPE + ROPE)


def ring(count, step):
    return [(i, (i + step) % count) for i in range(count)]


def rotate(values, positions):
    half_dim = values.shape[-1] // 2
    inv_freq = rope_base ** (-jnp.arange(half_dim, dtype=F32) * 2.0 / values.shape[-1])
    angles = positions.astype(F32)[:, None] * inv_freq[None, :]
    angles = angles.reshape((angles.shape[0],) + (1,) * (values.ndim - 2) + (half_dim,))
    cosine = jnp.cos(angles)
    sine_part = jnp.sin(angles)
    first_half = values[..., :half_dim].astype(F32)
    second_half = values[..., half_dim:].astype(F32)
    return jnp.concatenate(
        [
            first_half * cosine - second_half * sine_part,
            second_half * cosine + first_half * sine_part,
        ],
        axis=-1,
    )


def attend_body(where, own, other, first, second, *rest):
    earlier = rest[:-10]
    out, kbuf, vbuf, wk, wv, qs, tops, acc, sbuf, allkeys = rest[-10:]
    base = 0
    for part in earlier:
        base = part.shape[1]
        out[:, :base, :] = part[...]
    ep = where[0]
    tp = where[1]
    z = where[2]
    x = where[3]
    c = where[4]
    short = jnp.minimum(ep, N_EP - 1 - ep)
    n_short = short // TILE
    n_long = (N_EP - 1 - short) // TILE
    long_half = jnp.where(ep < N_EP // 2, 1, 0)
    heads = 4
    pieces = (first, second)
    allkeys[: N_EP // 2] = own[...]
    allkeys[N_EP // 2 :] = other[...]
    row = lax.broadcasted_iota(jnp.int32, (ROPE, 128), 0)
    lane = lax.broadcasted_iota(jnp.int32, (ROPE, 128), 1)
    pass_rope = jnp.where(lane == row + NOPE, 1.0, 0.0).astype(BF)
    lane = lax.broadcasted_iota(jnp.int32, (KVLAT, 128), 1)
    for h in range(heads):
        up = pieces[h // 2][384:512, (h % 2) * 128 : (h % 2 + 1) * 128]
        wk[:KVLAT, h * 128 : (h + 1) * 128] = jnp.where(lane < NOPE, up, jnp.zeros_like(up))
        wk[KVLAT:, h * 128 : (h + 1) * 128] = pass_rope
        wv[h * VDIM : (h + 1) * VDIM, :] = up.T[NOPE:, :]
    for half in range(2):
        for h in range(heads):
            at = (half * 2 + h % 2) * 96
            q = pieces[h // 2][at : at + 96, :].astype(F32) * score_scale
            high = q.astype(BF)
            low = (q - high.astype(F32)).astype(BF)
            pad = jnp.zeros((32, HALF), BF)
            qs[half, h] = jnp.concatenate([high, pad, low, pad], axis=0)
    tops[...] = jnp.full(tops.shape, neg_big, F32)
    acc[...] = jnp.zeros(acc.shape, F32)

    def project(t, _):
        blocks = []
        for b in range(TILE):
            zb = t // 2
            xb = (t % 2) * 2 + b // 2
            cb = b % 2
            at = ((c + cb) % 2) * 32 + ((x - xb) % 4) * 8 + (z - zb) % 8
            blocks.append(allkeys[at])
        turned = jnp.concatenate(blocks, axis=1)
        kbuf[t] = jnp.dot(turned.T, wk[...], preferred_element_type=F32).astype(BF)
        vbuf[t] = jnp.dot(wv[...], turned[:KVLAT], preferred_element_type=F32).astype(BF)
        return 0

    lax.fori_loop(0, n_long + 1, project, 0)
    ones = jnp.ones((16, TILE * PIECE), BF)

    def tile(t, half, at_edge):
        if at_edge:
            r = lax.broadcasted_iota(jnp.int32, (TILE * PIECE, HALF), 0)
            q = lax.broadcasted_iota(jnp.int32, (TILE * PIECE, HALF), 1)
            block = jnp.where(half == 0, ep, N_EP - 1 - ep)
            first_key = (r // PIECE) * 512 + r % PIECE
            allowed = (first_key - q) <= 512 * block + HALF * half - 2048 * t - PIECE * tp
        for h in range(heads):
            k = kbuf[t, :, h * 128 : (h + 1) * 128]
            scores = jnp.dot(
                jnp.concatenate([k, k], axis=1), qs[half, h], preferred_element_type=F32
            )
            if at_edge:
                scores = jnp.where(allowed, scores, neg_big)
            sbuf[h] = scores
        for h in range(heads):
            scores = sbuf[h]
            old = tops[half, h, 0:1, :]
            new = jnp.maximum(old, jnp.max(scores, axis=0, keepdims=True))
            probs = jnp.exp2(scores - new)
            if at_edge:
                probs = jnp.where(allowed, probs, 0.0)
            v = jnp.concatenate([vbuf[t, h * VDIM : (h + 1) * VDIM, :], ones], axis=0)
            part = jnp.dot(v, probs.astype(BF), preferred_element_type=F32)
            acc[half, h] = acc[half, h] * jnp.exp2(old - new) + part
            tops[half, h, 0:1, :] = new

    def inner(w, _):
        is_long = w < n_long
        tile(
            jnp.where(is_long, w, w - n_long),
            jnp.where(is_long, long_half, 1 - long_half),
            False,
        )
        return 0

    lax.fori_loop(0, n_long + n_short, inner, 0)

    def edge(w, _):
        tile(
            jnp.where(w == 0, n_long, n_short),
            jnp.where(w == 0, long_half, 1 - long_half),
            True,
        )
        return 0

    lax.fori_loop(0, 2, edge, 0)
    for half in range(2):
        parts = ([], [], [])
        for h in range(heads):
            a = acc[half, h]
            total = a[VDIM : VDIM + 1]
            seen = total > 0.0
            safe = jnp.where(seen, total, 1.0)
            o = (a[:VDIM] / safe).astype(BF)
            lse = jnp.where(seen, tops[half, h, 0:1, :] + jnp.log2(safe), neg_big)
            one = lse.astype(BF).astype(F32)
            two = (lse - one).astype(BF).astype(F32)
            parts[0].append(one)
            parts[1].append(two)
            parts[2].append(lse - one - two)
            for cc in range(2):
                to = (2 * half + cc - tp) % N_TP
                out[to, base + h * VDIM : base + (h + 1) * VDIM, :] = o[:, cc * 128 : (cc + 1) * 128]
        stats = jnp.concatenate(
            parts[0] + parts[1] + parts[2] + [jnp.zeros((4, HALF), F32)], axis=0
        ).astype(BF)
        for cc in range(2):
            to = (2 * half + cc - tp) % N_TP
            out[to, base + heads * VDIM : base + heads * VDIM + 16, :] = stats[:, cc * 128 : (cc + 1) * 128]


def attend(where, keys, first, second, *earlier):
    work = 17 * 4 * TILE * PIECE * HALF
    return pl.pallas_call(
        attend_body,
        out_shape=jax.ShapeDtypeStruct(
            (4, (4 * VDIM + 16) * (1 + len(earlier)), 128), BF
        ),
        in_specs=[pl.BlockSpec(memory_space=pltpu.SMEM)]
        + [pl.BlockSpec(memory_space=pltpu.VMEM)] * (4 + len(earlier)),
        out_specs=pl.BlockSpec(memory_space=pltpu.VMEM),
        scratch_shapes=[
            pltpu.VMEM((N_EP // TILE, TILE * PIECE, 4 * 128), BF),
            pltpu.VMEM((N_EP // TILE, 4 * VDIM, TILE * PIECE), BF),
            pltpu.VMEM((KVLAT + ROPE, 4 * 128), BF),
            pltpu.VMEM((4 * VDIM, KVLAT), BF),
            pltpu.VMEM((2, 4, 256, HALF), BF),
            pltpu.VMEM((2, 4, 8, HALF), F32),
            pltpu.VMEM((2, 4, VDIM + 16, HALF), F32),
            pltpu.VMEM((4, TILE * PIECE, HALF), F32),
            pltpu.VMEM((N_EP, KVLAT + ROPE, PIECE), BF),
        ],
        compiler_params=pltpu.CompilerParams(vmem_limit_bytes=36 * 1024 * 1024),
        cost_estimate=pl.CostEstimate(
            flops=work * 1000, bytes_accessed=4 << 20, transcendentals=work
        ),
        name="attend",
    )(where, *keys, first, second, *earlier)


def stack_body(*refs):
    for n, part in enumerate(refs[:-1]):
        refs[-1][n] = part[...]


def stack(parts):
    return pl.pallas_call(
        stack_body,
        out_shape=jax.ShapeDtypeStruct((len(parts), *parts[0].shape), BF),
        in_specs=[pl.BlockSpec(memory_space=pltpu.VMEM)] * len(parts),
        out_specs=pl.BlockSpec(memory_space=pltpu.VMEM),
        cost_estimate=pl.CostEstimate(flops=1 << 20, bytes_accessed=1 << 20, transcendentals=0),
        name="stack",
    )(*parts)


def join_body(*refs):
    out = refs[-1]
    got = refs[:-1]
    part = 4 * VDIM + 16
    for e in range(N_TP):
        for k in range(2):
            lses = []
            vals = []
            for d in range(N_TP):
                g = (e - d) % N_TP
                h = (g % 2) * 2 + k
                ref = got[d]
                at = (g // 2) * part
                stats = ref[at + 4 * VDIM : at + part, :].astype(F32)
                lses.append(stats[h : h + 1] + stats[4 + h : 5 + h] + stats[8 + h : 9 + h])
                vals.append(ref[at + h * VDIM : at + (h + 1) * VDIM, :].astype(F32))
            top = jnp.maximum(jnp.maximum(lses[0], lses[1]), jnp.maximum(lses[2], lses[3]))
            ws = [jnp.exp2(a - top) for a in lses]
            total = ws[0] + ws[1] + ws[2] + ws[3]
            o = ws[0] * vals[0] + ws[1] * vals[1] + ws[2] * vals[2] + ws[3] * vals[3]
            at = e * 128 + k * VDIM
            out[at : at + VDIM, :] = (o / total).astype(BF)


def join(pieces):
    return pl.pallas_call(
        join_body,
        out_shape=jax.ShapeDtypeStruct((512, 128), BF),
        in_specs=[pl.BlockSpec(memory_space=pltpu.VMEM)] * N_TP,
        out_specs=pl.BlockSpec(memory_space=pltpu.VMEM),
        cost_estimate=pl.CostEstimate(flops=1 << 20, bytes_accessed=1 << 20, transcendentals=0),
        name="join",
    )(*pieces)


def mix_body(attn, w0, w1, w2, w3, out):
    a = attn[...].T
    total = jnp.zeros((128, D), F32)
    for e, w in enumerate((w0, w1, w2, w3)):
        total = total + jnp.dot(
            a[:, e * 128 : (e + 1) * 128], w[...], preferred_element_type=F32
        )
    out[...] = total.astype(BF)


def mix(attn, weights):
    return pl.pallas_call(
        mix_body,
        out_shape=jax.ShapeDtypeStruct((128, D), BF),
        in_specs=[pl.BlockSpec(memory_space=pltpu.VMEM)] * 5,
        out_specs=pl.BlockSpec(memory_space=pltpu.VMEM),
        cost_estimate=pl.CostEstimate(
            flops=2 * 128 * 512 * D, bytes_accessed=3 << 20, transcendentals=0
        ),
        name="mix",
    )(attn, *weights)


def route_body(routes, turned, tokens, send, dest):
    experts = lax.broadcasted_iota(jnp.int32, (ROWS, N_EP), 1)
    a = lax.broadcasted_iota(jnp.int32, (ROWS, ROWS), 0)
    b = lax.broadcasted_iota(jnp.int32, (ROWS, ROWS), 1)
    before = jnp.where(b < a, 1.0, 0.0).astype(BF)
    named = [jnp.where(routes[:, k : k + 1] == experts, 1.0, 0.0) for k in range(2)]
    base = lax.broadcasted_iota(jnp.int32, (1, N_EP), 1).astype(F32) * SLOTS
    for k in range(2):
        rank = jnp.dot(before, named[k].astype(BF), preferred_element_type=F32) + base
        if k:
            rank = rank + jnp.sum(named[0], axis=0, keepdims=True)
        dest[:, k : k + 1] = jnp.sum(rank * named[k], axis=1, keepdims=True).astype(jnp.int32)
    experts = lax.broadcasted_iota(jnp.int32, (N_EP, ROWS), 0)
    before = jnp.where(a < b, 1.0, 0.0).astype(BF)
    named = [jnp.where(turned[k : k + 1, :] == experts, 1.0, 0.0) for k in range(2)]
    base = lax.broadcasted_iota(jnp.int32, (N_EP, 1), 0).astype(F32) * SLOTS
    slot = lax.broadcasted_iota(jnp.int32, (N_EP * SLOTS, ROWS), 0)
    pick = jnp.zeros((N_EP * SLOTS, ROWS), jnp.bool_)
    for k in range(2):
        rank = jnp.dot(named[k].astype(BF), before, preferred_element_type=F32) + base
        if k:
            rank = rank + jnp.sum(named[0], axis=1, keepdims=True)
        to = jnp.sum(rank * named[k], axis=0, keepdims=True).astype(jnp.int32)
        pick = pick | (slot == to)
    pick = jnp.where(pick, 1.0, 0.0).astype(BF)
    send[...] = jnp.dot(pick, tokens[...], preferred_element_type=F32).astype(BF)


def route(routes, tokens):
    return pl.pallas_call(
        route_body,
        out_shape=(
            jax.ShapeDtypeStruct((N_EP * SLOTS, tokens.shape[1]), BF),
            jax.ShapeDtypeStruct((ROWS, 2), jnp.int32),
        ),
        in_specs=[pl.BlockSpec(memory_space=pltpu.VMEM)] * 3,
        out_specs=(pl.BlockSpec(memory_space=pltpu.VMEM),) * 2,
        cost_estimate=pl.CostEstimate(flops=1 << 28, bytes_accessed=1 << 20, transcendentals=0),
        name="route",
    )(routes, routes.T, tokens)


def expert_body(
    where, x0, x1, x2, x3, gain, gate_w, up_w, down_w, out, xs, wg, wu, wd, gate, up, hidden, sems
):
    tp = where[1]
    quarter = D // N_TP

    def rows(d):
        return pl.ds(pl.multiple_of(((tp - d) % N_TP) * quarter, quarter), quarter)

    def cols(d):
        return pl.ds(pl.multiple_of(((tp + d) % N_TP) * quarter, quarter), quarter)

    def gate_copy(d):
        return pltpu.make_async_copy(gate_w.at[0, rows(d), :], wg.at[d], sems.at[0, d])

    def up_copy(d):
        return pltpu.make_async_copy(up_w.at[0, rows(d), :], wu.at[d], sems.at[1, d])

    def down_copy(d):
        return pltpu.make_async_copy(down_w.at[0, :, cols(d)], wd.at[d], sems.at[2, d])

    for d in range(N_TP):
        gate_copy(d).start()
        up_copy(d).start()
    for d in range(N_TP):
        down_copy(d).start()
    squares = jnp.zeros((x0.shape[0], 1), F32)
    for d, x in enumerate((x0, x1, x2, x3)):
        v = x[...].astype(F32)
        squares = squares + jnp.sum(v * v, axis=1, keepdims=True)
        xs[d] = (v * gain[pl.ds((tp - d) % N_TP, 1), :]).astype(BF)
    row_scale = lax.rsqrt(squares / D + eps)
    gate[...] = jnp.zeros(gate.shape, F32)
    up[...] = jnp.zeros(up.shape, F32)

    def inputs(d, _):
        gate_copy(d).wait()
        up_copy(d).wait()
        gate[...] += jnp.dot(xs[d], wg[d], preferred_element_type=F32)
        up[...] += jnp.dot(xs[d], wu[d], preferred_element_type=F32)
        return 0

    lax.fori_loop(0, N_TP, inputs, 0)
    g = gate[...] * row_scale
    hidden[...] = (g / (1.0 + jnp.exp(-g)) * (up[...] * row_scale)).astype(BF)

    def outputs(d, _):
        down_copy(d).wait()
        out[d] = jnp.dot(hidden[...], wd[d], preferred_element_type=F32).astype(BF)
        return 0

    lax.fori_loop(0, N_TP, outputs, 0)


def expert(where, xs, gain, gate_w, up_w, down_w):
    rows = xs[0].shape[0]
    hidden = gate_w.shape[2]
    quarter = D // N_TP
    return pl.pallas_call(
        expert_body,
        out_shape=jax.ShapeDtypeStruct((N_TP, rows, quarter), BF),
        in_specs=[pl.BlockSpec(memory_space=pltpu.SMEM)]
        + [pl.BlockSpec(memory_space=pltpu.VMEM)] * 5
        + [pl.BlockSpec(memory_space=pl.ANY)] * 3,
        out_specs=pl.BlockSpec(memory_space=pltpu.VMEM),
        scratch_shapes=[
            pltpu.VMEM((N_TP, rows, quarter), BF),
            pltpu.VMEM((N_TP, quarter, hidden), BF),
            pltpu.VMEM((N_TP, quarter, hidden), BF),
            pltpu.VMEM((N_TP, hidden, quarter), BF),
            pltpu.VMEM((rows, hidden), F32),
            pltpu.VMEM((rows, hidden), F32),
            pltpu.VMEM((rows, hidden), BF),
            pltpu.SemaphoreType.DMA((3, N_TP)),
        ],
        compiler_params=pltpu.CompilerParams(vmem_limit_bytes=40 * 1024 * 1024),
        cost_estimate=pl.CostEstimate(
            flops=6 * rows * D * hidden, bytes_accessed=16 << 20, transcendentals=rows * hidden
        ),
        name="expert",
    )(where, *xs, gain.reshape(N_TP, quarter), gate_w, up_w, down_w)


def weigh_body(dest, weights, back, out):
    slot = lax.broadcasted_iota(jnp.int32, (ROWS, N_EP * SLOTS), 1)
    w = jnp.zeros((ROWS, N_EP * SLOTS), F32)
    for k in range(2):
        w = jnp.where(slot == dest[:, k : k + 1], weights[:, k : k + 1], w)
    high = w.astype(BF)
    rest = w - high.astype(F32)
    mid = rest.astype(BF)
    low = (rest - mid.astype(F32)).astype(BF)
    b = back[...]
    total = jnp.dot(low, b, preferred_element_type=F32)
    total = total + jnp.dot(mid, b, preferred_element_type=F32)
    total = total + jnp.dot(high, b, preferred_element_type=F32)
    out[...] = total.astype(BF)


def weigh(dest, weights, back):
    return pl.pallas_call(
        weigh_body,
        out_shape=jax.ShapeDtypeStruct((ROWS, back.shape[1]), BF),
        in_specs=[pl.BlockSpec(memory_space=pltpu.VMEM)] * 3,
        out_specs=pl.BlockSpec(memory_space=pltpu.VMEM),
        cost_estimate=pl.CostEstimate(flops=1 << 29, bytes_accessed=1 << 20, transcendentals=0),
        name="weigh",
    )(dest, weights, back)


def from_each(value, axis, count):
    return [value] + [lax.ppermute(value, axis, ring(count, d)) for d in range(1, count)]


def layer(
    queries,
    kv_latent,
    rope_key,
    kv_gain,
    kv_up,
    mix_out,
    moe_in,
    moe_gain,
    routes,
    route_weights,
    gate_w,
    up_w,
    down_w,
):
    ep = lax.axis_index(EP)
    tp = lax.axis_index("tp")
    where = jnp.stack(
        [ep, tp, lax.axis_index("z"), lax.axis_index("x"), lax.axis_index("c")]
    ).astype(jnp.int32)

    key_index = ep * 512 + tp * PIECE + jnp.arange(PIECE, dtype=jnp.int32)
    latent = kv_latent.astype(F32)
    normed = (
        latent * lax.rsqrt(jnp.mean(latent * latent, axis=-1, keepdims=True) + eps) * kv_gain
    ).astype(BF)
    key_rot = rotate(rope_key, key_index).astype(BF)
    keys = jnp.concatenate([normed.T, key_rot.T], axis=0)
    keys = from_each(keys, "z", 8)
    keys = stack(keys)
    keys = from_each(keys, "x", 4)
    keys = stack(keys).reshape(N_EP // 2, KVLAT + ROPE, PIECE)
    keys = [keys, lax.ppermute(keys, "c", ring(2, 1))]

    query_index = ep * 512 + jnp.arange(512, dtype=jnp.int32)
    query_rot = rotate(queries[..., NOPE:], query_index).astype(BF)
    q = jnp.concatenate([queries[..., :NOPE], query_rot], axis=-1).transpose(1, 2, 0)
    mirrored = lax.ppermute(q[:, :, HALF:], EP, [(i, N_EP - 1 - i) for i in range(N_EP)])
    bundle = jnp.concatenate(
        [q[:, :, :HALF].reshape(192, HALF), mirrored.reshape(192, HALF), kv_up.reshape(128, 256)],
        axis=0,
    )
    send, dest = route(routes, moe_in)
    arrived = lax.all_to_all(
        send.reshape(N_EP, SLOTS * 4, 128), EP, split_axis=0, concat_axis=0, tiled=True
    )
    arrived = arrived.reshape(N_EP * SLOTS, 512)
    bundles = from_each(bundle, "tp", N_TP)
    mix_w = from_each(mix_out.reshape(128, D), "tp", N_TP)
    arrived, mix_w = lax.optimization_barrier((arrived, mix_w))
    xs = from_each(arrived, "tp", N_TP)
    part_a = attend(where, keys, bundles[0], bundles[1])
    xs, part_a = lax.optimization_barrier((xs, part_a))
    results = expert(where, xs, moe_gain, gate_w, up_w, down_w)
    results, bundles = lax.optimization_barrier((results, bundles))
    sums = [results[0]] + [
        lax.ppermute(results[d], "tp", ring(N_TP, d)) for d in range(1, N_TP)
    ]
    parts = attend(where, keys, bundles[2], bundles[3], part_a)
    sums, _ = lax.optimization_barrier((sums, parts))

    def owner(i, j):
        return (i if j < 2 else N_EP - 1 - i) * N_TP + j

    got = [
        lax.ppermute(
            parts[d],
            ALL,
            [(i * N_TP + j, owner(i, (j + d) % N_TP)) for i in range(N_EP) for j in range(N_TP)],
        )
        for d in range(N_TP)
    ]
    summed = sum(a.astype(F32) for a in sums).astype(BF)
    summed = summed.reshape(N_EP, SLOTS * 4, 128)
    back = lax.all_to_all(summed, EP, split_axis=0, concat_axis=0, tiled=True)
    moe_out = weigh(dest, route_weights, back.reshape(N_EP * SLOTS, 512))

    attn = join(got)
    mixed = mix(attn, mix_w)
    return (mixed, moe_out)


def solution(mesh):
    split = Mesh(mesh.devices.reshape(8, 4, 2, mesh.shape["tp"]), ALL)
    placed = (
        P(EP, "tp", None),
        P(ALL, None),
        P(ALL, None),
        P(),
        P(None, "tp", None),
        P("tp", None, None),
        P(EP, "tp"),
        P(),
        P(EP, None),
        P(EP, None),
        P(EP, None, "tp"),
        P(EP, None, "tp"),
        P(EP, "tp", None),
    )
    return jax.shard_map(
        layer,
        mesh=split,
        in_specs=placed,
        out_specs=(P(ALL, None), P(EP, "tp")),
        check_vma=False,
    )
```
